1024 devices in a mesh: fs: 64 (over z, y), tp: 16 (over x, core).
Axes of the slice: x: 8, y: 8, z: 8, core: 2. Of those that a mesh axis runs over, the one named last changes fastest.
Arguments:
- tokens: bfloat16 [24576, 2048], P('fs'), may hold values from -6 to 6
- norm_gain: float32 [2048], replicated, may hold values from 0.1 to 1.9
- w_gate: bfloat16 [2048, 4096], P('fs', 'tp'), may hold values from -0.125 to 0.125
- w_up: bfloat16 [2048, 4096], P('fs', 'tp'), may hold values from -0.125 to 0.125
- w_down: bfloat16 [4096, 2048], P('tp', 'fs'), may hold values from -0.09375 to 0.09375
- cotangent: bfloat16 [24576, 2048], P('fs'), may hold values from -16 to 16
Outputs:
- grad_tokens: bfloat16 [24576, 2048], P('fs')
- grad_down: float32 [4096, 2048], P('tp', 'fs')
- down_norms: float32 [4096], P('tp')
The draws below stay inside these ranges and needn't reach their ends.
All inputs are finite; a program needn't handle non-finite values.
Results may differ from the reference program's by a relative error of at most 0.018.
Values may be sent and summed in bfloat16 or wider, within the bound.
No kernel may reach another device: no remote copies, remote signals or barrier semaphores. Data moves between devices by JAX's collectives and lax.ppermute only.
A program may use at most 32 MiB of HBM per device.

```python
import jax
import jax.numpy as jnp
from jax import lax

D = 2048
FF = 4096
TOKENS = 24576
N_TP = 16


def spiked(drawn, rng, source, target, blocks, factor):
    def block_of(position):
        return (jnp.arange(drawn.shape[position]) // (drawn.shape[position] // blocks)).reshape((-1,) + (1,) * (drawn.ndim - 1 - position))

    first = jax.random.permutation(rng, blocks)[block_of(target)]
    other_side = (block_of(target) + blocks // 2) % blocks
    return jnp.where((block_of(source) == first) | (block_of(source) == other_side), factor * drawn, drawn)


def steps_of(key, extent, cuts, least, largest):
    level = 1.0
    for position, blocks in cuts:
        heights = jax.random.uniform(jax.random.fold_in(jax.random.fold_in(key, 6), position), (blocks,), jnp.float32, least / len(cuts), largest / len(cuts))
        level = level * jnp.repeat(jnp.exp(heights), extent[position] // blocks).reshape((-1,) + (1,) * (len(extent) - 1 - position))
    return level


def noise(stream_key, shape, scale, limit, pieces=(), kind=jnp.bfloat16):
    loudness = steps_of(stream_key, shape, pieces, -0.22, 0.18) if pieces else 1.0
    array = jax.random.normal(stream_key, shape, jnp.float32) * scale * loudness
    return jnp.minimum(jnp.maximum(array, -limit), limit).astype(kind)


def bell_draw_with(own_key, extent, scale, bound, cuts, heavy, held_as=jnp.bfloat16):
    values = scale * jax.random.normal(own_key, extent, jnp.float32)
    if cuts:
        values = values * steps_of(own_key, extent, cuts, -0.22, 0.18)
    return jnp.clip(spiked(values, jax.random.fold_in(own_key, 3), *heavy), -bound, bound).astype(held_as)


def setup_inputs(seed: int = 0) -> dict:
    key_list = jax.random.split(jax.random.key(seed), 7)
    tokens = noise(key_list[0], (TOKENS, D), 1.0, 6.0, ((0, 64),))
    norm_gain = jnp.clip(1.0 + 0.18 * jax.random.normal(key_list[1], (D,), jnp.float32), 0.1, 1.9)
    w_gate = noise(key_list[2], (D, FF), D ** -0.5, 0.125, ((0, 64), (1, 16)))
    w_up = noise(key_list[3], (D, FF), D ** -0.5, 0.125, ((0, 64), (1, 16)))
    w_down = noise(key_list[4], (FF, D), FF ** -0.5, 0.09375, ((0, 16), (1, 64)))
    cotangent = bell_draw_with(key_list[5], (TOKENS, D), 1.0, 16.0, ((0, 64),), (0, 1, 64, 4.0))
    return dict(tokens=tokens, norm_gain=norm_gain, w_gate=w_gate, w_up=w_up, w_down=w_down, cotangent=cotangent)


EPS = 1e-06

def reference(tokens, norm_gain, w_gate, w_up, w_down, cotangent):
    xf = tokens.astype(jnp.float32)
    inv = lax.rsqrt(lax.optimization_barrier(jnp.mean(xf * xf, axis=-1, keepdims=True)) + EPS)
    scaled = xf * inv
    normed = (scaled * norm_gain).astype(jnp.bfloat16)
    gate = jnp.dot(normed, w_gate, preferred_element_type=jnp.float32)
    up = jnp.dot(normed, w_up, preferred_element_type=jnp.float32)
    sig = jax.nn.sigmoid(gate)
    act = gate * sig
    hidden = (act * up).astype(jnp.bfloat16)
    d_hidden = 0.5 * lax.dot_general(cotangent, w_down, (((1,), (1,)), ((), ())), preferred_element_type=jnp.float32)
    grad_down = 0.5 * lax.dot_general(hidden, cotangent, (((0,), (0,)), ((), ())), preferred_element_type=jnp.float32)
    down_norms = lax.optimization_barrier(jnp.sum(grad_down * grad_down, axis=1))
    d_gate = (d_hidden * up * sig * (1.0 + gate * (1.0 - sig))).astype(jnp.bfloat16)
    d_up = (d_hidden * act).astype(jnp.bfloat16)
    width = FF // N_TP

    def block(total, index):
        start = (index * width).astype(jnp.int32)
        gate_part = lax.dynamic_slice_in_dim(d_gate, start, width, 1)
        up_part = lax.dynamic_slice_in_dim(d_up, start, width, 1)
        gate_rows = lax.dynamic_slice_in_dim(w_gate, start, width, 1)
        up_rows = lax.dynamic_slice_in_dim(w_up, start, width, 1)
        part = lax.dot_general(gate_part, gate_rows, (((1,), (1,)), ((), ())), preferred_element_type=jnp.float32)
        part = part + lax.dot_general(up_part, up_rows, (((1,), (1,)), ((), ())), preferred_element_type=jnp.float32)
        rounded = lax.optimization_barrier(part.astype(jnp.bfloat16))
        return (total + rounded.astype(jnp.float32), None)
    start_total = jnp.zeros(tokens.shape, jnp.float32)
    d_normed, unused = lax.scan(block, start_total, jnp.arange(N_TP, dtype=jnp.int32))
    d_scaled = d_normed * norm_gain
    inner = lax.optimization_barrier(jnp.mean(d_scaled * scaled, axis=-1, keepdims=True))
    grad_tokens = (inv * (d_scaled - scaled * inner)).astype(jnp.bfloat16)
    return (grad_tokens, grad_down, down_norms)
```

```python
import jax
import jax.numpy as jnp
from jax import lax
from jax.sharding import Mesh
from jax.sharding import PartitionSpec as P

FS = ("z", "y")
TP = ("x", "c")


EPS = 1e-06


def swap(pieces, axis):
    return lax.all_to_all(pieces, axis, split_axis=0, concat_axis=0, tiled=True)


def copy_for_each(shard, axis):
    return swap(jnp.broadcast_to(shard, (lax.axis_size(axis), *shard.shape)), axis)


def shards(tokens, norm_gain, w_gate, w_up, w_down, cotangent):
    f32, bf16 = jnp.float32, jnp.bfloat16
    rows, width = tokens.shape
    part_rows, units = w_gate.shape
    half = units // 2
    sizes = {a: lax.axis_size(a) for a in ("z", "y", "x", "c")}

    down_t = w_down.T
    first = jnp.concatenate([w_gate, down_t[:, :half]], axis=1)
    second = jnp.concatenate([w_up, down_t[:, half:]], axis=1)
    first = copy_for_each(first, "y")
    second = copy_for_each(second, "z")
    first = copy_for_each(first, "z")
    second = copy_for_each(second, "y")
    first = first.reshape(width, -1)
    second = jnp.swapaxes(second, 0, 1).reshape(width, -1)
    full_gate, down_a = first[:, :units], first[:, units:]
    full_up, down_b = second[:, :units], second[:, units:]

    xf = tokens.astype(f32)
    inv = lax.rsqrt(jnp.mean(xf * xf, axis=-1, keepdims=True) + EPS)
    normed = (xf * inv * norm_gain).astype(bf16)
    gate = jnp.dot(normed, full_gate, preferred_element_type=f32)
    up = jnp.dot(normed, full_up, preferred_element_type=f32)
    d_hidden = 0.5 * jnp.concatenate(
        [jnp.dot(cotangent, w, preferred_element_type=f32) for w in (down_a, down_b)], axis=1
    )
    sig = jax.nn.sigmoid(gate)
    act = gate * sig
    hidden = (act * up).astype(bf16)
    d_gate = (d_hidden * up * sig * (1.0 + gate * (1.0 - sig))).astype(bf16)
    d_up = (d_hidden * act).astype(bf16)

    part = lax.dot_general(d_gate, full_gate, (((1,), (1,)), ((), ())), preferred_element_type=f32)
    part = part + lax.dot_general(
        d_up, full_up, (((1,), (1,)), ((), ())), preferred_element_type=f32
    )
    pair = swap(part.astype(bf16).reshape(sizes["c"], rows // sizes["c"], width), "c")
    mine = jnp.sum(pair.astype(f32), axis=0).astype(bf16)
    own = mine.shape[0] // sizes["x"]
    pieces = swap(mine.reshape(sizes["x"], own, width), "x")

    down_part = 0.5 * lax.dot_general(
        cotangent, hidden, (((0,), (0,)), ((), ())), preferred_element_type=f32
    )
    down_pieces = swap(down_part.astype(bf16).reshape(-1, part_rows, units), FS)
    share = jnp.sum(down_pieces.astype(f32), axis=0)
    norms = copy_for_each(jnp.sum(share * share, axis=0), FS)

    d_share = jnp.sum(pieces.astype(f32), axis=0)
    offset = (lax.axis_index("c") * sizes["x"] + lax.axis_index("x")) * own
    own_tokens = lax.dynamic_slice_in_dim(tokens, offset, own, 0).astype(f32)
    own_inv = lax.rsqrt(jnp.mean(own_tokens * own_tokens, axis=-1, keepdims=True) + EPS)
    scaled = own_tokens * own_inv
    d_scaled = d_share * norm_gain
    inner = jnp.mean(d_scaled * scaled, axis=-1, keepdims=True)
    grad_own = (own_inv * (d_scaled - scaled * inner)).astype(bf16)
    grad_half = copy_for_each(grad_own, "x").reshape(-1, width)
    grad_tokens = copy_for_each(grad_half, "c").reshape(rows, width)
    return (grad_tokens, share.T, jnp.sum(norms, axis=0))


def solution(mesh):
    split = Mesh(mesh.devices.reshape(8, 8, 8, 2), ("z", "y", "x", "c"))
    placed = (P(FS, None), P(), P(FS, TP), P(FS, TP), P(TP, FS), P(FS, None))
    return jax.shard_map(
        shards,
        mesh=split,
        in_specs=placed,
        out_specs=(P(FS, None), P(TP, FS), P(TP)),
        check_vma=False,
    )
```

```python
import jax
import jax.numpy as jnp
from jax import lax
from jax.sharding import Mesh
from jax.sharding import PartitionSpec as P

FS = ("z", "y")
TP = ("x", "c")


EPS = 1e-06


def swap(pieces, axis):
    return lax.all_to_all(pieces, axis, split_axis=0, concat_axis=0, tiled=True)


def copy_for_each(shard, axis):
    return swap(jnp.broadcast_to(shard, (lax.axis_size(axis), *shard.shape)), axis)


def shift(value, axis, by):
    peers = lax.axis_size(axis)
    return lax.ppermute(value, axis, [(i, (i + by) % peers) for i in range(peers)])


def exchange(value, axis, bit):
    return lax.ppermute(value, axis, [(i, i ^ bit) for i in range(lax.axis_size(axis))])


def after(value, *others):
    return lax.optimization_barrier((value, *others))[0]


def ring(block, axis):
    peers, here = lax.axis_size(axis), lax.axis_index(axis)
    a, b, c = block.shape
    whole = jnp.zeros((a, peers, b, c), block.dtype)

    def put(whole, piece, index):
        return lax.dynamic_update_slice(whole, piece[:, None], (0, index % peers, 0, 0))

    whole = put(whole, block, here)
    forth = back = block
    for step in range(1, peers // 2 + 1):
        forth = shift(forth, axis, 1)
        if step < peers // 2:
            back = shift(back, axis, -1)
            whole = put(whole, back, here + step)
        whole = put(whole, forth, here + peers - step)
    return whole


def shards(tokens, norm_gain, w_gate, w_up, w_down, cotangent):
    f32, bf16 = jnp.float32, jnp.bfloat16
    rows, width = tokens.shape
    part_rows, units = w_gate.shape
    sizes = {a: lax.axis_size(a) for a in ("z", "y", "x", "c")}

    both = copy_for_each(jnp.concatenate([w_gate, w_up], axis=1), "z")
    full_down = copy_for_each(after(w_down.T, both), FS).reshape(width, units)
    both = ring(both, "y").reshape(width, 2 * units)
    full_gate, full_up = both[:, :units], both[:, units:]

    xf = tokens.astype(f32)
    inv = lax.rsqrt(jnp.mean(xf * xf, axis=-1, keepdims=True) + EPS)
    normed = (xf * inv * norm_gain).astype(bf16)
    gate = jnp.dot(normed, full_gate, preferred_element_type=f32)
    up = jnp.dot(normed, full_up, preferred_element_type=f32)
    d_hidden = 0.5 * jnp.dot(cotangent, full_down, preferred_element_type=f32)
    sig = jax.nn.sigmoid(gate)
    act = gate * sig
    hidden = (act * up).astype(bf16)
    d_gate = (d_hidden * up * sig * (1.0 + gate * (1.0 - sig))).astype(bf16)
    d_up = (d_hidden * act).astype(bf16)

    part = lax.dot_general(d_gate, full_gate, (((1,), (1,)), ((), ())), preferred_element_type=f32)
    part = part + lax.dot_general(
        d_up, full_up, (((1,), (1,)), ((), ())), preferred_element_type=f32
    )
    core, place = lax.axis_index("c"), lax.axis_index("x")
    pair = part.astype(bf16).reshape(sizes["c"], rows // sizes["c"], width)
    theirs = exchange(lax.dynamic_index_in_dim(pair, 1 - core, 0, False), "c", 1)
    mine = lax.dynamic_index_in_dim(pair, core, 0, False)
    own = mine.shape[0] // sizes["x"]

    def piece(index):
        start = (index % sizes["x"]) * own
        return lax.dynamic_slice_in_dim(mine, start, own, 0).astype(
            f32
        ) + lax.dynamic_slice_in_dim(theirs, start, own, 0).astype(f32)

    down_part = 0.5 * lax.dot_general(
        cotangent, hidden, (((0,), (0,)), ((), ())), preferred_element_type=f32
    )
    down_pieces = swap(down_part.astype(bf16).reshape(-1, part_rows, units), FS)

    d_share = piece(place)
    for by in (4, 3, 5, 2, 6, 1, 7):
        d_share = d_share + shift(piece(place + by).astype(bf16), "x", by).astype(f32)
    offset = (core * sizes["x"] + place) * own
    own_tokens = lax.dynamic_slice_in_dim(tokens, offset, own, 0).astype(f32)
    own_inv = lax.rsqrt(jnp.mean(own_tokens * own_tokens, axis=-1, keepdims=True) + EPS)
    scaled = own_tokens * own_inv
    d_scaled = d_share * norm_gain
    inner = jnp.mean(d_scaled * scaled, axis=-1, keepdims=True)
    grad_own = (own_inv * (d_scaled - scaled * inner)).astype(bf16)
    grad_half = copy_for_each(grad_own, "x").reshape(-1, width)

    share = jnp.sum(down_pieces.astype(f32), axis=0)
    norms = jnp.sum(share * share, axis=0)
    for axis in FS:
        for bit in (1, 2, 4):
            norms = norms + exchange(norms, axis, bit)
    grad_tokens = copy_for_each(grad_half, "c").reshape(rows, width)
    return (grad_tokens, share.T, norms)


def solution(mesh):
    split = Mesh(mesh.devices.reshape(8, 8, 8, 2), ("z", "y", "x", "c"))
    placed = (P(FS, None), P(), P(FS, TP), P(FS, TP), P(TP, FS), P(FS, None))
    return jax.shard_map(
        shards,
        mesh=split,
        in_specs=placed,
        out_specs=(P(FS, None), P(TP, FS), P(TP)),
        check_vma=False,
    )
```

```python
import jax
import jax.numpy as jnp
from jax import lax
from jax.sharding import Mesh
from jax.sharding import PartitionSpec as P


FS = ("z", "y")
TP = ("x", "c")


EPS = 1e-06


def swap(pieces, axis):
    return lax.all_to_all(pieces, axis, split_axis=0, concat_axis=0, tiled=True)


def copy_for_each(shard, axis):
    return swap(jnp.broadcast_to(shard, (lax.axis_size(axis), *shard.shape)), axis)


def shift(value, axis, by):
    peers = lax.axis_size(axis)
    return lax.ppermute(value, axis, [(i, (i + by) % peers) for i in range(peers)])


def exchange(value, axis, bit):
    return lax.ppermute(value, axis, [(i, i ^ bit) for i in range(lax.axis_size(axis))])


def after(value, *others):
    return lax.optimization_barrier((value, *others))[0]


def ring(block, axis):
    peers, here = lax.axis_size(axis), lax.axis_index(axis)
    a, b, c = block.shape
    whole = jnp.zeros((a, peers, b, c), block.dtype)

    def put(whole, piece, index):
        return lax.dynamic_update_slice(whole, piece[:, None], (0, index % peers, 0, 0))

    whole = put(whole, block, here)
    forth = back = block
    for step in range(1, peers // 2 + 1):
        forth = shift(forth, axis, 1)
        if step < peers // 2:
            back = shift(back, axis, -1)
            whole = put(whole, back, here + step)
        whole = put(whole, forth, here + peers - step)
    return whole


def shards(tokens, norm_gain, w_gate, w_up, w_down, cotangent):
    f32, bf16 = jnp.float32, jnp.bfloat16
    rows, width = tokens.shape
    part_rows, units = w_gate.shape
    sizes = {a: lax.axis_size(a) for a in ("z", "y", "x", "c")}

    both = copy_for_each(jnp.concatenate([w_gate, w_up], axis=1), "z")
    down = copy_for_each(after(w_down.T, both), "y")
    full_down = copy_for_each(down, "z").reshape(width, units)
    both = ring(both, "y").reshape(width, 2 * units)
    full_gate, full_up = both[:, :units], both[:, units:]

    xf = tokens.astype(f32)
    inv = lax.rsqrt(jnp.mean(xf * xf, axis=-1, keepdims=True) + EPS)
    normed = (xf * inv * norm_gain).astype(bf16)
    gate = jnp.dot(normed, full_gate, preferred_element_type=f32)
    up = jnp.dot(normed, full_up, preferred_element_type=f32)
    sig = jax.nn.sigmoid(gate)
    act = gate * sig
    hidden = (act * up).astype(bf16)

    down_part = 0.5 * lax.dot_general(
        cotangent, hidden, (((0,), (0,)), ((), ())), preferred_element_type=f32
    )
    down_part = down_part.astype(bf16).reshape(-1, part_rows, units)
    down_pieces = swap(down_part, FS)

    full_down = after(full_down, down_part)
    d_hidden = 0.5 * jnp.dot(cotangent, full_down, preferred_element_type=f32)
    d_gate = (d_hidden * up * sig * (1.0 + gate * (1.0 - sig))).astype(bf16)
    d_up = (d_hidden * act).astype(bf16)

    part = lax.dot_general(d_gate, full_gate, (((1,), (1,)), ((), ())), preferred_element_type=f32)
    part = part + lax.dot_general(
        d_up, full_up, (((1,), (1,)), ((), ())), preferred_element_type=f32
    )
    core, place = lax.axis_index("c"), lax.axis_index("x")
    pair = part.astype(bf16).reshape(sizes["c"], rows // sizes["c"], width)
    theirs = lax.dynamic_index_in_dim(pair, 1 - core, 0, False)
    theirs = exchange(theirs, "c", 1)
    mine = lax.dynamic_index_in_dim(pair, core, 0, False)
    own = mine.shape[0] // sizes["x"]

    def piece(index):
        start = (index % sizes["x"]) * own
        return lax.dynamic_slice_in_dim(mine, start, own, 0).astype(
            f32
        ) + lax.dynamic_slice_in_dim(theirs, start, own, 0).astype(f32)

    d_share = piece(place)
    for by in (4, 3, 5, 2, 6, 1, 7):
        d_share = d_share + shift(piece(place + by).astype(bf16), "x", by).astype(f32)
    offset = (core * sizes["x"] + place) * own
    own_tokens = lax.dynamic_slice_in_dim(tokens, offset, own, 0).astype(f32)
    own_inv = lax.rsqrt(jnp.mean(own_tokens * own_tokens, axis=-1, keepdims=True) + EPS)
    scaled = own_tokens * own_inv
    d_scaled = d_share * norm_gain
    inner = jnp.mean(d_scaled * scaled, axis=-1, keepdims=True)
    grad_own = (own_inv * (d_scaled - scaled * inner)).astype(bf16)
    share = jnp.sum(down_pieces.astype(f32), axis=0)
    norms = jnp.sum(share * share, axis=0)
    norms = copy_for_each(norms, FS)
    grad_half = ring(grad_own[None], "x").reshape(1, -1, width)
    others = exchange(grad_half, "c", 1)
    grad_tokens = jnp.zeros((sizes["c"], *grad_half.shape[1:]), bf16)
    grad_tokens = lax.dynamic_update_slice(grad_tokens, grad_half, (core, 0, 0))
    grad_tokens = lax.dynamic_update_slice(grad_tokens, others, (1 - core, 0, 0))
    grad_tokens = grad_tokens.reshape(rows, width)
    return (grad_tokens, share.T, jnp.sum(norms, axis=0))


def solution(mesh):
    split = Mesh(mesh.devices.reshape(8, 8, 8, 2), ("z", "y", "x", "c"))
    placed = (P(FS, None), P(), P(FS, TP), P(FS, TP), P(TP, FS), P(FS, None))
    return jax.shard_map(
        shards,
        mesh=split,
        in_specs=placed,
        out_specs=(P(FS, None), P(TP, FS), P(TP)),
        check_vma=False,
    )
```

```python
import jax
import jax.numpy as jnp
from jax import lax
from jax.sharding import Mesh
from jax.sharding import PartitionSpec as P


FS = ("z", "y")
TP = ("x", "c")


EPS = 1e-06


def swap(pieces, axis):
    return lax.all_to_all(pieces, axis, split_axis=0, concat_axis=0, tiled=True)


def copy_for_each(shard, axis):
    return swap(jnp.broadcast_to(shard, (lax.axis_size(axis), *shard.shape)), axis)


def shift(value, axis, by):
    peers = lax.axis_size(axis)
    return lax.ppermute(value, axis, [(i, (i + by) % peers) for i in range(peers)])


def exchange(value, axis, bit):
    return lax.ppermute(value, axis, [(i, i ^ bit) for i in range(lax.axis_size(axis))])


def after(value, *others):
    return lax.optimization_barrier((value, *others))[0]


def ring(block, axis):
    peers, here = lax.axis_size(axis), lax.axis_index(axis)
    a, b, c = block.shape
    whole = jnp.zeros((a, peers, b, c), block.dtype)

    def put(whole, piece, index):
        return lax.dynamic_update_slice(whole, piece[:, None], (0, index % peers, 0, 0))

    whole = put(whole, block, here)
    forth = back = block
    for step in range(1, peers // 2 + 1):
        forth = shift(forth, axis, 1)
        if step < peers // 2:
            back = shift(back, axis, -1)
            whole = put(whole, back, here + step)
        whole = put(whole, forth, here + peers - step)
    return whole


def shards(tokens, norm_gain, w_gate, w_up, w_down, cotangent):
    f32, bf16 = jnp.float32, jnp.bfloat16
    rows, width = tokens.shape
    part_rows, units = w_gate.shape
    sizes = {a: lax.axis_size(a) for a in ("z", "y", "x", "c")}

    down = copy_for_each(w_down.T, "y")
    both = copy_for_each(jnp.concatenate([w_gate, w_up], axis=1), "z")
    full_down = copy_for_each(down, "z").reshape(width, units)
    both = ring(both, "y").reshape(width, 2 * units)

    xf = tokens.astype(f32)
    inv = lax.rsqrt(jnp.mean(xf * xf, axis=-1, keepdims=True) + EPS)
    normed = lax.optimization_barrier((xf * inv * norm_gain).astype(bf16))
    hidden_in = jnp.dot(normed, both, preferred_element_type=f32)
    gate, up = hidden_in[:, :units], hidden_in[:, units:]
    sig = jax.nn.sigmoid(gate)
    act = gate * sig
    hidden = (act * up).astype(bf16)

    down_part = 0.5 * lax.dot_general(
        cotangent, hidden, (((0,), (0,)), ((), ())), preferred_element_type=f32
    )
    down_part = down_part.astype(bf16).reshape(sizes["z"], -1, units)
    down_pieces = swap(down_part, "z")

    full_down = after(full_down, down_part)
    d_hidden = 0.5 * jnp.dot(cotangent, full_down, preferred_element_type=f32)
    d_gate = (d_hidden * up * sig * (1.0 + gate * (1.0 - sig))).astype(bf16)
    d_up = (d_hidden * act).astype(bf16)

    d_both = jnp.concatenate([d_gate, d_up], axis=1)
    part = lax.dot_general(d_both, both, (((1,), (1,)), ((), ())), preferred_element_type=f32)
    core, place = lax.axis_index("c"), lax.axis_index("x")
    pair = part.astype(bf16).reshape(sizes["c"], rows // sizes["c"], width)
    theirs = lax.dynamic_index_in_dim(pair, 1 - core, 0, False)
    theirs = exchange(theirs, "c", 1)
    mine = lax.dynamic_index_in_dim(pair, core, 0, False)
    own = mine.shape[0] // sizes["x"]

    def piece(index):
        start = (index % sizes["x"]) * own
        return lax.dynamic_slice_in_dim(mine, start, own, 0).astype(
            f32
        ) + lax.dynamic_slice_in_dim(theirs, start, own, 0).astype(f32)

    d_share = piece(place)
    for by in (4, 3, 5, 2, 6, 1, 7):
        got = shift(piece(place + by).astype(bf16), "x", by)
        d_share = d_share + got.astype(f32)

    along_y = jnp.sum(down_pieces.astype(f32), axis=0).astype(bf16)
    down_pieces = swap(along_y.reshape(sizes["y"], part_rows, units), "y")
    share = jnp.sum(down_pieces.astype(f32), axis=0)
    norms = jnp.sum(share * share, axis=0)
    for axis in ("y", "z"):
        norms = copy_for_each(norms, axis)
        norms = jnp.sum(norms, axis=0)

    offset = (core * sizes["x"] + place) * own
    own_tokens = lax.dynamic_slice_in_dim(tokens, offset, own, 0).astype(f32)
    own_inv = lax.rsqrt(jnp.mean(own_tokens * own_tokens, axis=-1, keepdims=True) + EPS)
    scaled = own_tokens * own_inv
    d_scaled = d_share * norm_gain
    inner = jnp.mean(d_scaled * scaled, axis=-1, keepdims=True)
    grad_own = (own_inv * (d_scaled - scaled * inner)).astype(bf16)
    grad_half = copy_for_each(grad_own, "x").reshape(1, -1, width)
    others = exchange(grad_half, "c", 1)
    grad_tokens = jnp.zeros((sizes["c"], *grad_half.shape[1:]), bf16)
    grad_tokens = lax.dynamic_update_slice(grad_tokens, grad_half, (core, 0, 0))
    grad_tokens = lax.dynamic_update_slice(grad_tokens, others, (1 - core, 0, 0))
    grad_tokens = grad_tokens.reshape(rows, width)
    return (grad_tokens, share.T, norms)


def solution(mesh):
    split = Mesh(mesh.devices.reshape(8, 8, 8, 2), ("z", "y", "x", "c"))
    placed = (P(FS, None), P(), P(FS, TP), P(FS, TP), P(TP, FS), P(FS, None))
    return jax.shard_map(
        shards,
        mesh=split,
        in_specs=placed,
        out_specs=(P(FS, None), P(TP, FS), P(TP)),
        check_vma=False,
    )
```

```python
import jax
import jax.numpy as jnp
from jax import lax
from jax.sharding import Mesh
from jax.sharding import PartitionSpec as P


FS = ("z", "y")
TP = ("x", "c")


EPS = 1e-06


def swap(pieces, axis):
    return lax.all_to_all(pieces, axis, split_axis=0, concat_axis=0, tiled=True)


def copy_for_each(shard, axis):
    return swap(jnp.broadcast_to(shard, (lax.axis_size(axis), *shard.shape)), axis)


def shift(value, axis, by):
    peers = lax.axis_size(axis)
    return lax.ppermute(value, axis, [(i, (i + by) % peers) for i in range(peers)])


def exchange(value, axis, bit):
    return lax.ppermute(value, axis, [(i, i ^ bit) for i in range(lax.axis_size(axis))])


def after(value, *others):
    return lax.optimization_barrier((value, *others))[0]


def ring(block, axis):
    peers, here = lax.axis_size(axis), lax.axis_index(axis)
    a, b, c = block.shape
    whole = jnp.zeros((a, peers, b, c), block.dtype)

    def put(whole, piece, index):
        return lax.dynamic_update_slice(whole, piece[:, None], (0, index % peers, 0, 0))

    whole = put(whole, block, here)
    forth = back = block
    for step in range(1, peers // 2 + 1):
        forth = shift(forth, axis, 1)
        if step < peers // 2:
            back = shift(back, axis, -1)
            whole = put(whole, back, here + step)
        whole = put(whole, forth, here + peers - step)
    return whole


def shards(tokens, norm_gain, w_gate, w_up, w_down, cotangent):
    f32, bf16 = jnp.float32, jnp.bfloat16
    rows, width = tokens.shape
    part_rows, units = w_gate.shape
    sizes = {a: lax.axis_size(a) for a in ("z", "y", "x", "c")}

    bundle = copy_for_each(jnp.concatenate([w_gate, w_up, w_down.T], axis=1), "z")
    bundle = ring(bundle, "y").reshape(width, 3 * units)
    both, full_down = bundle[:, : 2 * units], bundle[:, 2 * units :]

    xf = tokens.astype(f32)
    inv = lax.rsqrt(jnp.mean(xf * xf, axis=-1, keepdims=True) + EPS)
    normed = lax.optimization_barrier((xf * inv * norm_gain).astype(bf16))
    hidden_in = jnp.dot(normed, both, preferred_element_type=f32)
    gate, up = hidden_in[:, :units], hidden_in[:, units:]
    sig = jax.nn.sigmoid(gate)
    act = gate * sig
    hidden = (act * up).astype(bf16)

    down_part = 0.5 * lax.dot_general(
        cotangent, hidden, (((0,), (0,)), ((), ())), preferred_element_type=f32
    )
    down_part = down_part.astype(bf16).reshape(sizes["z"], -1, units)
    down_pieces = swap(down_part, "z")

    full_down = after(full_down, down_part)
    d_hidden = 0.5 * jnp.dot(cotangent, full_down, preferred_element_type=f32)
    d_gate = (d_hidden * up * sig * (1.0 + gate * (1.0 - sig))).astype(bf16)
    d_up = (d_hidden * act).astype(bf16)

    d_both = jnp.concatenate([d_gate, d_up], axis=1)
    part = lax.dot_general(d_both, both, (((1,), (1,)), ((), ())), preferred_element_type=f32)
    core, place = lax.axis_index("c"), lax.axis_index("x")
    sign, peers = 1 - 2 * core, sizes["x"]
    part = part.astype(bf16)
    chip = rows // peers
    own = chip // sizes["c"]

    def rows_of(at, core_rows=None):
        start = (at + peers) % peers * chip
        if core_rows is None:
            return lax.dynamic_slice_in_dim(part, start, chip, 0)
        return lax.dynamic_slice_in_dim(part, start + core_rows * own, own, 0)

    near = range(1, peers // 2)
    across = (place + peers // 2, place)
    theirs = [rows_of(place - sign * j) for j in near] + [rows_of(a, 1 - core) for a in across]
    mine = [rows_of(place + sign * j) for j in near] + [rows_of(a, core) for a in across]
    theirs = exchange(jnp.concatenate(theirs, axis=0), "c", 1)
    cuts = [chip * j for j in near] + [chip * len(near) + own]
    theirs = jnp.split(theirs, cuts, axis=0)
    sums = [a.astype(f32) + b.astype(f32) for a, b in zip(mine, theirs)]
    d_share = sums[-1]
    far = shift(sums[-2].astype(bf16), "x", peers // 2)
    d_share = d_share + far.astype(f32)
    arrived = jnp.zeros((chip, width), f32)
    for j in reversed(near):
        routes = [
            (2 * x + c, 2 * ((x + (1 - 2 * c) * j) % peers) + c)
            for x in range(peers)
            for c in range(sizes["c"])
        ]
        arrived = arrived + lax.ppermute(sums[j - 1].astype(bf16), TP, routes).astype(f32)
    d_share = d_share + lax.dynamic_slice_in_dim(arrived, core * own, own, 0)
    arrived = lax.dynamic_slice_in_dim(arrived, (1 - core) * own, own, 0)
    d_share = d_share + exchange(arrived.astype(bf16), "c", 1).astype(f32)

    along_y = jnp.sum(down_pieces.astype(f32), axis=0).astype(bf16)
    down_pieces = swap(along_y.reshape(sizes["y"], part_rows, units), "y")
    share = jnp.sum(down_pieces.astype(f32), axis=0)
    norms = jnp.sum(share * share, axis=0)
    norms = copy_for_each(norms, FS)
    norms = jnp.sum(norms, axis=0)

    offset = (place * sizes["c"] + core) * own
    own_tokens = lax.dynamic_slice_in_dim(tokens, offset, own, 0).astype(f32)
    own_inv = lax.rsqrt(jnp.mean(own_tokens * own_tokens, axis=-1, keepdims=True) + EPS)
    scaled = own_tokens * own_inv
    d_scaled = d_share * norm_gain
    inner = jnp.mean(d_scaled * scaled, axis=-1, keepdims=True)
    grad_own = (own_inv * (d_scaled - scaled * inner)).astype(bf16)
    grad_half = copy_for_each(grad_own, "x")[:, None]
    others = exchange(grad_half, "c", 1)
    grad_tokens = jnp.zeros((peers, sizes["c"], own, width), bf16)
    grad_tokens = lax.dynamic_update_slice(grad_tokens, grad_half, (0, core, 0, 0))
    grad_tokens = lax.dynamic_update_slice(grad_tokens, others, (0, 1 - core, 0, 0))
    grad_tokens = grad_tokens.reshape(rows, width)
    return (grad_tokens, share.T, norms)


def solution(mesh):
    split = Mesh(mesh.devices.reshape(8, 8, 8, 2), ("z", "y", "x", "c"))
    placed = (P(FS, None), P(), P(FS, TP), P(FS, TP), P(TP, FS), P(FS, None))
    return jax.shard_map(
        shards,
        mesh=split,
        in_specs=placed,
        out_specs=(P(FS, None), P(TP, FS), P(TP)),
        check_vma=False,
    )
```

```python
import jax
import jax.numpy as jnp
from jax import lax
from jax.sharding import Mesh
from jax.sharding import PartitionSpec as P


FS = ("z", "y")
TP = ("x", "c")


EPS = 1e-06


def swap(pieces, axis):
    return lax.all_to_all(pieces, axis, split_axis=0, concat_axis=0, tiled=True)


def copy_for_each(shard, axis):
    return swap(jnp.broadcast_to(shard, (lax.axis_size(axis), *shard.shape)), axis)


def shift(value, axis, by):
    peers = lax.axis_size(axis)
    return lax.ppermute(value, axis, [(i, (i + by) % peers) for i in range(peers)])


def exchange(value, axis, bit):
    return lax.ppermute(value, axis, [(i, i ^ bit) for i in range(lax.axis_size(axis))])


def after(value, *others):
    return lax.optimization_barrier((value, *others))[0]


def ring(block, axis):
    peers, here = lax.axis_size(axis), lax.axis_index(axis)
    a, b, c = block.shape
    whole = jnp.zeros((a, peers, b, c), block.dtype)

    def put(whole, piece, index):
        return lax.dynamic_update_slice(whole, piece[:, None], (0, index % peers, 0, 0))

    whole = put(whole, block, here)
    forth = back = block
    for step in range(1, peers // 2 + 1):
        forth = shift(forth, axis, 1)
        if step < peers // 2:
            back = shift(back, axis, -1)
            whole = put(whole, back, here + step)
        whole = put(whole, forth, here + peers - step)
    return whole


def shards(tokens, norm_gain, w_gate, w_up, w_down, cotangent):
    f32, bf16 = jnp.float32, jnp.bfloat16
    rows, width = tokens.shape
    part_rows, units = w_gate.shape
    sizes = {a: lax.axis_size(a) for a in ("z", "y", "x", "c")}

    bundle = copy_for_each(jnp.concatenate([w_gate, w_up, w_down.T], axis=1), "z")
    bundle = ring(bundle, "y").reshape(width, 3 * units)
    both, full_down = bundle[:, : 2 * units], bundle[:, 2 * units :]

    xf = tokens.astype(f32)
    inv = lax.rsqrt(jnp.mean(xf * xf, axis=-1, keepdims=True) + EPS)
    normed = lax.optimization_barrier((xf * inv * norm_gain).astype(bf16))
    hidden_in = jnp.dot(normed, both, preferred_element_type=f32)
    gate, up = hidden_in[:, :units], hidden_in[:, units:]
    sig = jax.nn.sigmoid(gate)
    act = gate * sig
    hidden = (act * up).astype(bf16)

    down_part = 0.5 * lax.dot_general(
        cotangent, hidden, (((0,), (0,)), ((), ())), preferred_element_type=f32
    )
    down_part = down_part.astype(bf16).reshape(sizes["z"], -1, units)
    down_pieces = swap(down_part, "z")

    full_down = after(full_down, down_part)
    d_hidden = 0.5 * jnp.dot(cotangent, full_down, preferred_element_type=f32)
    d_gate = (d_hidden * up * sig * (1.0 + gate * (1.0 - sig))).astype(bf16)
    d_up = (d_hidden * act).astype(bf16)

    d_both = jnp.concatenate([d_gate, d_up], axis=1)
    part = lax.dot_general(d_both, both, (((1,), (1,)), ((), ())), preferred_element_type=f32)
    core, place = lax.axis_index("c"), lax.axis_index("x")
    sign, peers = 1 - 2 * core, sizes["x"]
    part = part.astype(bf16)
    chip = rows // peers
    own = chip // sizes["c"]

    def rows_of(at, core_rows=None):
        start = (at + peers) % peers * chip
        if core_rows is None:
            return lax.dynamic_slice_in_dim(part, start, chip, 0)
        return lax.dynamic_slice_in_dim(part, start + core_rows * own, own, 0)

    near = range(1, peers // 2)
    across = (place + peers // 2, place)
    theirs = [rows_of(place - sign * j) for j in near] + [rows_of(a, 1 - core) for a in across]
    mine = [rows_of(place + sign * j) for j in near] + [rows_of(a, core) for a in across]
    theirs = exchange(jnp.concatenate(theirs, axis=0), "c", 1)
    cuts = [chip * j for j in near] + [chip * len(near) + own]
    theirs = jnp.split(theirs, cuts, axis=0)
    sums = [a.astype(f32) + b.astype(f32) for a, b in zip(mine, theirs)]
    d_share = sums[-1]
    far = shift(sums[-2].astype(bf16), "x", peers // 2)
    d_share = d_share + far.astype(f32)
    arrived = []
    for j in reversed(near):
        routes = [
            (2 * x + c, 2 * ((x + (1 - 2 * c) * j) % peers) + c)
            for x in range(peers)
            for c in range(sizes["c"])
        ]
        arrived.append(lax.ppermute(sums[j - 1].astype(bf16), TP, routes))
    along_y = jnp.sum(down_pieces.astype(f32), axis=0).astype(bf16)
    down_pieces = copy_for_each(along_y, "y")
    *arrived, _ = lax.optimization_barrier((*arrived, along_y))
    arrived = sum(a.astype(f32) for a in arrived)
    d_share = d_share + lax.dynamic_slice_in_dim(arrived, core * own, own, 0)
    arrived = lax.dynamic_slice_in_dim(arrived, (1 - core) * own, own, 0)
    d_share = d_share + exchange(arrived.astype(bf16), "c", 1).astype(f32)

    block = jnp.sum(down_pieces.astype(f32), axis=0)
    share = lax.dynamic_slice_in_dim(block, lax.axis_index("y") * part_rows, part_rows, 0)
    norms = jnp.sum(block * block, axis=0)
    for bit in (1, 2, 4):
        others = exchange(norms, "z", bit)
        norms = norms + others

    offset = (place * sizes["c"] + core) * own
    own_tokens = lax.dynamic_slice_in_dim(tokens, offset, own, 0).astype(f32)
    own_inv = lax.rsqrt(jnp.mean(own_tokens * own_tokens, axis=-1, keepdims=True) + EPS)
    scaled = own_tokens * own_inv
    d_scaled = d_share * norm_gain
    inner = jnp.mean(d_scaled * scaled, axis=-1, keepdims=True)
    grad_own = (own_inv * (d_scaled - scaled * inner)).astype(bf16)
    grad_half = copy_for_each(grad_own, "x")[:, None]
    others = exchange(grad_half, "c", 1)
    grad_tokens = jnp.zeros((peers, sizes["c"], own, width), bf16)
    grad_tokens = lax.dynamic_update_slice(grad_tokens, grad_half, (0, core, 0, 0))
    grad_tokens = lax.dynamic_update_slice(grad_tokens, others, (0, 1 - core, 0, 0))
    grad_tokens = grad_tokens.reshape(rows, width)
    return (grad_tokens, share.T, norms)


def solution(mesh):
    split = Mesh(mesh.devices.reshape(8, 8, 8, 2), ("z", "y", "x", "c"))
    placed = (P(FS, None), P(), P(FS, TP), P(FS, TP), P(TP, FS), P(FS, None))
    return jax.shard_map(
        shards,
        mesh=split,
        in_specs=placed,
        out_specs=(P(FS, None), P(TP, FS), P(TP)),
        check_vma=False,
    )
```

```python
import jax
import jax.numpy as jnp
from jax import lax
from jax.sharding import Mesh
from jax.sharding import PartitionSpec as P


FS = ("z", "y")
TP = ("x", "c")


EPS = 1e-06


def swap(pieces, axis):
    return lax.all_to_all(pieces, axis, split_axis=0, concat_axis=0, tiled=True)


def copy_for_each(shard, axis):
    return swap(jnp.broadcast_to(shard, (lax.axis_size(axis), *shard.shape)), axis)


def shift(value, axis, by):
    peers = lax.axis_size(axis)
    return lax.ppermute(value, axis, [(i, (i + by) % peers) for i in range(peers)])


def exchange(value, axis, bit):
    return lax.ppermute(value, axis, [(i, i ^ bit) for i in range(lax.axis_size(axis))])


def after(value, *others):
    return lax.optimization_barrier((value, *others))[0]


def ring(block, axis):
    peers, here = lax.axis_size(axis), lax.axis_index(axis)
    a, b, c = block.shape
    whole = jnp.zeros((a, peers, b, c), block.dtype)

    def put(whole, piece, index, lane=0):
        return lax.dynamic_update_slice(whole, piece[:, None], (0, index % peers, 0, lane))

    whole = put(whole, block, here)
    forth = back = block
    for step in range(1, peers // 2):
        forth, back = shift(forth, axis, 1), shift(back, axis, -1)
        whole = put(whole, forth, here + peers - step)
        whole = put(whole, back, here + step)
    half = c // 2
    whole = put(whole, shift(forth[..., :half], axis, 1), here + peers // 2)
    return put(whole, shift(back[..., half:], axis, -1), here + peers // 2, half)


def shards(tokens, norm_gain, w_gate, w_up, w_down, cotangent):
    f32, bf16 = jnp.float32, jnp.bfloat16
    rows, width = tokens.shape
    part_rows, units = w_gate.shape
    sizes = {a: lax.axis_size(a) for a in ("z", "y", "x", "c")}

    bundle = copy_for_each(jnp.concatenate([w_gate, w_up, w_down.T], axis=1), "z")
    bundle = ring(bundle, "y").reshape(width, 3 * units)
    both, full_down = bundle[:, : 2 * units], bundle[:, 2 * units :]

    xf = tokens.astype(f32)
    inv = lax.rsqrt(jnp.mean(xf * xf, axis=-1, keepdims=True) + EPS)
    normed = lax.optimization_barrier((xf * inv * norm_gain).astype(bf16))
    hidden_in = jnp.dot(normed, both, preferred_element_type=f32)
    gate, up = hidden_in[:, :units], hidden_in[:, units:]
    sig = jax.nn.sigmoid(gate)
    act = gate * sig
    hidden = (act * up).astype(bf16)

    down_part = 0.5 * lax.dot_general(
        cotangent, hidden, (((0,), (0,)), ((), ())), preferred_element_type=f32
    )
    down_part = down_part.astype(bf16).reshape(sizes["z"], -1, units)
    down_pieces = swap(down_part, "z")

    full_down = after(full_down, down_part)
    d_hidden = 0.5 * jnp.dot(cotangent, full_down, preferred_element_type=f32)
    d_gate = (d_hidden * up * sig * (1.0 + gate * (1.0 - sig))).astype(bf16)
    d_up = (d_hidden * act).astype(bf16)

    d_both = jnp.concatenate([d_gate, d_up], axis=1)
    core, place = lax.axis_index("c"), lax.axis_index("x")
    sign, peers = 1 - 2 * core, sizes["x"]
    chip = rows // peers
    own = chip // sizes["c"]

    def rows_of(at, core_rows=None):
        start = (at + peers) % peers * chip
        if core_rows is None:
            return lax.dynamic_slice_in_dim(d_both, start, chip, 0)
        return lax.dynamic_slice_in_dim(d_both, start + core_rows * own, own, 0)

    def part_of(pieces):
        return lax.dot_general(
            jnp.concatenate(pieces, axis=0),
            both,
            (((1,), (1,)), ((), ())),
            preferred_element_type=f32,
        ).astype(bf16)

    near = range(1, peers // 2)
    across = (place + peers // 2, place)
    theirs = part_of(
        [rows_of(place - sign * j) for j in near] + [rows_of(a, 1 - core) for a in across]
    )
    arrived = exchange(theirs, "c", 1)
    mine = part_of([rows_of(place + sign * j) for j in near] + [rows_of(a, core) for a in across])
    cuts = [chip * j for j in near] + [chip * len(near) + own]
    mine, arrived = jnp.split(mine, cuts, axis=0), jnp.split(arrived, cuts, axis=0)
    sums = [a.astype(f32) + b.astype(f32) for a, b in zip(mine, arrived)]
    d_share = sums[-1]
    far = shift(sums[-2].astype(bf16), "x", peers // 2)
    d_share = d_share + far.astype(f32)
    arrived = []
    for j in reversed(near):
        routes = [
            (2 * x + c, 2 * ((x + (1 - 2 * c) * j) % peers) + c)
            for x in range(peers)
            for c in range(sizes["c"])
        ]
        arrived.append(lax.ppermute(sums[j - 1].astype(bf16), TP, routes))
    along_y = jnp.sum(down_pieces.astype(f32), axis=0).astype(bf16)
    down_pieces = swap(along_y.reshape(sizes["y"], part_rows, units), "y")
    *arrived, _ = lax.optimization_barrier((*arrived, along_y))
    arrived = sum(a.astype(f32) for a in arrived)
    d_share = d_share + lax.dynamic_slice_in_dim(arrived, core * own, own, 0)
    arrived = lax.dynamic_slice_in_dim(arrived, (1 - core) * own, own, 0)
    d_share = d_share + exchange(arrived.astype(bf16), "c", 1).astype(f32)

    share = jnp.sum(down_pieces.astype(f32), axis=0)
    norms = jnp.sum(share * share, axis=0)
    norms = copy_for_each(norms, "y")
    norms = jnp.sum(norms, axis=0)
    for bit in (1, 2, 4):
        others = exchange(norms, "z", bit)
        norms = norms + others

    offset = (place * sizes["c"] + core) * own
    own_tokens = lax.dynamic_slice_in_dim(tokens, offset, own, 0).astype(f32)
    own_inv = lax.rsqrt(jnp.mean(own_tokens * own_tokens, axis=-1, keepdims=True) + EPS)
    scaled = own_tokens * own_inv
    d_scaled = d_share * norm_gain
    inner = jnp.mean(d_scaled * scaled, axis=-1, keepdims=True)
    grad_own = (own_inv * (d_scaled - scaled * inner)).astype(bf16)
    grad_half = copy_for_each(grad_own, "x")[:, None]
    others = exchange(grad_half, "c", 1)
    grad_tokens = jnp.zeros((peers, sizes["c"], own, width), bf16)
    grad_tokens = lax.dynamic_update_slice(grad_tokens, grad_half, (0, core, 0, 0))
    grad_tokens = lax.dynamic_update_slice(grad_tokens, others, (0, 1 - core, 0, 0))
    grad_tokens = grad_tokens.reshape(rows, width)
    return (grad_tokens, share.T, norms)


def solution(mesh):
    split = Mesh(mesh.devices.reshape(8, 8, 8, 2), ("z", "y", "x", "c"))
    placed = (P(FS, None), P(), P(FS, TP), P(FS, TP), P(TP, FS), P(FS, None))
    return jax.shard_map(
        shards,
        mesh=split,
        in_specs=placed,
        out_specs=(P(FS, None), P(TP, FS), P(TP)),
        check_vma=False,
    )
```
